512 devices in a mesh: sp: 64 (over z, y), tp: 8 (over x, core).
Axes of the slice: x: 4, y: 8, z: 8, core: 2. Of those that a mesh axis runs over, the one named last changes fastest.
Arguments:
- tokens: bfloat16 [16384, 4096], P('sp', 'tp'), may hold values from -480 to 480
- gain: float32 [4096], P('tp'), may hold values from 0.1 to 1.9
- q_att: bfloat16 [4096, 2048], P('sp', 'tp'), may hold values from -2.90625 to 2.90625
- k_att: bfloat16 [4096, 1024], P('sp', 'tp'), may hold values from -0.09375 to 0.09375
- v_att: bfloat16 [4096, 1024], P('sp', 'tp'), may hold values from -0.75 to 0.75
- q_ret: bfloat16 [4096, 1024], P('sp', 'tp'), may hold values from -0.09375 to 0.09375
- k_ret: bfloat16 [4096, 1024], P('sp', 'tp'), may hold values from -0.09375 to 0.09375
- v_ret: bfloat16 [4096, 1024], P('sp', 'tp'), may hold values from -0.09375 to 0.09375
- out_att: bfloat16 [2048, 4096], P('tp', 'sp'), may hold values from -0.109375 to 0.109375
- out_ret: bfloat16 [1024, 4096], P('tp', 'sp'), may hold values from -0.109375 to 0.109375
- sink: float32 [16], P('tp'), may hold values from 3 to 7
- decay_log: float32 [8, 16384], P('tp', 'sp'), may hold values from -2.125 to 0
Outputs:
- mixed: bfloat16 [16384, 4096], P(('sp', 'tp'))
- log_weight: float32 [16, 16384], P('tp', 'sp')
The draws below stay inside these ranges and needn't reach their ends.
All inputs are finite; a program needn't handle non-finite values.
Results may differ from the reference program's by a relative error of at most 0.017.
Values may be sent and summed in bfloat16 or wider, within the bound.
A program may use at most 128 MiB of HBM per device.

```python
import jax
import jax.numpy as jnp
from jax import lax

D = 4096
ATT_HEADS = 16
KV_HEADS = 8
RET_HEADS = 8
HEAD_DIM = 128
SPAN_RADIUS = 128
TOK_DEV = 256
TOKENS = 16384
N_TP = 8


def drawn_pair(key):
    base = jax.random.fold_in(key, 31)
    lookup_fraction = jnp.clip(jax.random.normal(jax.random.fold_in(base, 1), (D, KV_HEADS * HEAD_DIM), jnp.float32), -6.0, 6.0) * D ** (-0.5)
    query_part = jnp.clip(jax.random.normal(jax.random.fold_in(base, 2), (D, ATT_HEADS * HEAD_DIM), jnp.float32), -6.0, 6.0) * D ** (-0.5)
    return (query_part, lookup_fraction)


def draw_q_att(key, part):
    return drawn_pair(key)[0].astype(jnp.bfloat16)


def draw_k_att(key, part):
    return drawn_pair(key)[1].astype(jnp.bfloat16)


def draw_tokens(key, part):
    normal_part = jnp.clip(jax.random.normal(jax.random.fold_in(key, 41), (TOKENS, D), jnp.float32), -6.0, 6.0)
    column = jnp.arange(D).astype(jnp.float32) / D
    course = 2.0 * (jnp.arange(TOKENS).astype(jnp.float32) + 0.5) / TOKENS - 1.0
    direction = jax.random.uniform(jax.random.fold_in(key, 43), (1, D), jnp.float32, -1.0, 1.0)
    drift = jnp.exp(1.2 * direction * course[:, None])
    scale = drift * (4.0 ** column)[None, :]
    return (normal_part * scale).astype(jnp.bfloat16)


def draw_decay_log(key, part):
    blocks = TOKENS // TOK_DEV
    share = 0.5
    fast = jax.random.uniform(jax.random.fold_in(key, 51), (RET_HEADS, 1), jnp.float32) < share
    fast_rate = jax.random.uniform(jax.random.fold_in(key, 52), (RET_HEADS, 1), jnp.float32, 10.0, 16.0) / TOK_DEV
    slow_rate = jax.random.uniform(jax.random.fold_in(key, 53), (RET_HEADS, 1), jnp.float32, 0.1, 0.3) / TOKENS
    fading_pace = jnp.where(fast, fast_rate, slow_rate)
    scaling_factor = jnp.exp(jax.random.uniform(jax.random.fold_in(key, 54), (RET_HEADS, blocks), jnp.float32, jnp.log(0.5), jnp.log(2.0)))
    scaling_factor = jnp.repeat(scaling_factor, TOK_DEV, axis=1)
    spots = jax.random.randint(jax.random.fold_in(key, 55), (2,), 0, TOKENS)
    agreement_tally = (jnp.arange(TOKENS)[None, :] == spots[:, None]).astype(jnp.float32)
    discarded_entries = jnp.log(jax.random.uniform(jax.random.fold_in(key, 56), (2, RET_HEADS), jnp.float32, 0.5, 0.8))
    clustered_lists = jnp.dot(discarded_entries.T, agreement_tally)
    return -fading_pace * scaling_factor + clustered_lists


def steps_of(key, dims, cuts, least, largest):
    loudness, own = 1.0, jax.random.fold_in(key, 6)
    for axis_at, shards_of in cuts:
        heights = jnp.exp(jax.random.uniform(jax.random.fold_in(own, axis_at), (shards_of,), jnp.float32, least / len(cuts), largest / len(cuts)))
        loudness = loudness * jnp.repeat(heights, dims[axis_at] // shards_of).reshape([-1 if axis == axis_at else 1 for axis in range(len(dims))])
    return loudness


def scatter_about(key, extent, spread, reach, split=(), kind=jnp.bfloat16):
    values = jax.random.normal(key, extent, jnp.float32) * spread
    if len(split) > 0:
        values = steps_of(key, extent, split, -0.22, 0.18) * values
    return jnp.clip(values, min=-reach, max=reach).astype(kind)


def setup_inputs(seed: int = 0) -> dict:
    streams_of = jax.random.split(jax.random.key(seed), 13)
    return {
        "tokens": draw_tokens(jax.random.fold_in(streams_of[12], 71), 0),
        "gain": jnp.clip(1.0 + 0.18 * jax.random.normal(streams_of[1], (D,), jnp.float32), 0.1, 1.9),
        "q_att": draw_q_att(jax.random.fold_in(streams_of[12], 71), 0),
        "k_att": draw_k_att(jax.random.fold_in(streams_of[12], 71), 0),
        "v_att": scatter_about(streams_of[4], (D, KV_HEADS * HEAD_DIM), (max(D // 64, 1)) ** -0.5, 0.75, ((0, 64), (1, 8))),
        "q_ret": scatter_about(streams_of[5], (D, RET_HEADS * HEAD_DIM), D ** -0.5, 0.09375, ((0, 64), (1, 8))),
        "k_ret": scatter_about(streams_of[6], (D, RET_HEADS * HEAD_DIM), D ** -0.5, 0.09375, ((0, 64), (1, 8))),
        "v_ret": scatter_about(streams_of[7], (D, RET_HEADS * HEAD_DIM), D ** -0.5, 0.09375, ((0, 64), (1, 8))),
        "out_att": scatter_about(streams_of[8], (ATT_HEADS * HEAD_DIM, D), ((ATT_HEADS + RET_HEADS) * HEAD_DIM) ** -0.5, 0.109375, ((0, 8), (1, 64))),
        "out_ret": scatter_about(streams_of[9], (RET_HEADS * HEAD_DIM, D), ((ATT_HEADS + RET_HEADS) * HEAD_DIM) ** -0.5, 0.109375, ((0, 8), (1, 64))),
        "sink": jnp.clip(3.0 + 4.0 * jax.random.uniform(streams_of[10], (ATT_HEADS,), jnp.float32) ** steps_of(streams_of[10], (ATT_HEADS,), ((0, 8),), -0.2, 0.2), 3.0, 7.0),
        "decay_log": draw_decay_log(jax.random.fold_in(streams_of[12], 71), 0),
    }


def rotate(values, angles):
    half = values.shape[-1] // 2
    first = values[..., :half]
    second = values[..., half:]
    cosine = jnp.cos(angles)[:, None, :]
    sine = jnp.sin(angles)[:, None, :]
    return jnp.concatenate([first * cosine - second * sine, second * cosine + first * sine], axis=-1)

def angle_table(positions):
    freqs = 10000.0 ** (-jnp.arange(0, HEAD_DIM, 2).astype(jnp.float32) / HEAD_DIM)
    return positions[:, None] * freqs[None, :]

def window_attention(queries, padded_keys, padded_values, sink_logit, offset, total_rows, block_rows):
    count = queries.shape[0] // block_rows
    nearby_memory = queries.shape[1]
    group = queries.shape[2]

    def single_block(index):
        begin = index * block_rows
        block_query = lax.dynamic_slice_in_dim(queries, begin, block_rows, 0).astype(jnp.float32)
        block_keys = lax.dynamic_slice_in_dim(padded_keys, begin, block_rows + 2 * SPAN_RADIUS, 0).astype(jnp.float32)
        block_values = lax.dynamic_slice_in_dim(padded_values, begin, block_rows + 2 * SPAN_RADIUS, 0).astype(jnp.float32)
        scores = jnp.einsum('qhgd,khd->hgqk', block_query, block_keys) * HEAD_DIM ** (-0.5)
        query_pos = offset + begin + jnp.arange(block_rows, dtype=jnp.int32)
        key_pos = offset + begin - SPAN_RADIUS + jnp.arange(block_rows + 2 * SPAN_RADIUS, dtype=jnp.int32)
        spacing = key_pos[None, :] - query_pos[:, None]
        valid = (jnp.abs(spacing) <= SPAN_RADIUS) & (key_pos >= 0)[None, :] & (key_pos < total_rows)[None, :]
        masked = jnp.where(valid, scores, -jnp.inf)
        top = jnp.maximum(lax.optimization_barrier(jnp.max(masked, axis=-1)), sink_logit[:, :, None])
        expo = jnp.exp(masked - top[..., None])
        total = lax.optimization_barrier(jnp.sum(expo, axis=-1)) + jnp.exp(sink_logit[:, :, None] - top)
        logs = top + jnp.log(total)
        probs = (expo / total[..., None]).astype(jnp.bfloat16)
        result = jnp.einsum('hgqk,khd->qhgd', probs.astype(jnp.float32), block_values).astype(jnp.bfloat16)
        return (result.reshape(block_rows, nearby_memory * group * HEAD_DIM), logs.reshape(nearby_memory * group, block_rows))
    outs, logs = lax.map(single_block, jnp.arange(count, dtype=jnp.int32))
    return (outs.reshape(queries.shape[0], -1), jnp.moveaxis(logs, 0, 1).reshape(logs.shape[1], -1))

def retention(queries, keys, values, decay):
    blocks = queries.shape[0] // TOK_DEV
    heads = queries.shape[1]
    highest = lax.Precision.HIGHEST
    query_b = queries.reshape(blocks, TOK_DEV, heads, HEAD_DIM)
    key_b = keys.reshape(blocks, TOK_DEV, heads, HEAD_DIM)
    value_b = values.reshape(blocks, TOK_DEV, heads, HEAD_DIM)
    decay_b = jnp.moveaxis(decay.reshape(heads, blocks, TOK_DEV), 1, 0)

    def local(items):
        query_f = items[0].astype(jnp.float32)
        key_f = items[1].astype(jnp.float32)
        value_f = items[2].astype(jnp.float32)
        cumul = jnp.cumsum(items[3], axis=1)
        last = cumul[:, -1]
        scores = jnp.einsum('qhd,khd->hqk', query_f, key_f)
        weights = jnp.exp(-jnp.abs(cumul[:, :, None] - cumul[:, None, :]))
        inner = jnp.einsum('hqk,khd->qhd', scores * weights, value_f, precision=highest)
        forward = jnp.einsum('hk,khd,khe->hde', jnp.exp(last[:, None] - cumul), key_f, value_f, precision=highest)
        backward = jnp.einsum('hk,khd,khe->hde', jnp.exp(cumul), key_f, value_f, precision=highest)
        return (inner, forward, backward, jnp.exp(last), cumul)
    inner, forward, backward, totals, cumuls = lax.map(local, (query_b, key_b, value_b, decay_b))

    def step(carry, item):
        return (item[0][:, None, None] * carry + item[1], carry)
    zero = jnp.zeros(forward.shape[1:], jnp.float32)
    _, before = lax.scan(step, zero, (totals, forward))
    _, after = lax.scan(step, zero, (totals, backward), reverse=True)
    query_f = query_b.astype(jnp.float32)
    lead = jnp.moveaxis(jnp.exp(cumuls), 1, 2)[..., None]
    trail = jnp.moveaxis(jnp.exp(cumuls[:, :, -1:] - cumuls), 1, 2)[..., None]
    carried = lead * jnp.einsum('bqhd,bhde->bqhe', query_f, before, precision=highest)
    carried = carried + trail * jnp.einsum('bqhd,bhde->bqhe', query_f, after, precision=highest)
    blended_output = inner + carried
    middle_point = blended_output - lax.optimization_barrier(jnp.mean(blended_output, axis=-1, keepdims=True))
    normed = middle_point * lax.rsqrt(lax.optimization_barrier(jnp.mean(middle_point * middle_point, axis=-1, keepdims=True)) + 1e-06)
    return normed.astype(jnp.bfloat16).reshape(queries.shape[0], heads * HEAD_DIM)

def reference(tokens, gain, q_att, k_att, v_att, q_ret, k_ret, v_ret, out_att, out_ret, sink, decay_log):
    widened = tokens.astype(jnp.float32)
    inverse = lax.rsqrt(lax.optimization_barrier(jnp.sum(widened * widened, axis=1)) / D + 1e-06)[:, None]
    scaled = (widened * gain).astype(jnp.bfloat16)

    def project(weight):
        return jnp.dot(scaled, weight, preferred_element_type=jnp.float32) * inverse
    angles = angle_table(jnp.arange(TOKENS).astype(jnp.float32))
    group = ATT_HEADS // KV_HEADS
    att_query = rotate(project(q_att).reshape(TOKENS, ATT_HEADS, HEAD_DIM), angles).astype(jnp.bfloat16)
    att_key = rotate(project(k_att).reshape(TOKENS, KV_HEADS, HEAD_DIM), angles).astype(jnp.bfloat16)
    att_value = project(v_att).astype(jnp.bfloat16).reshape(TOKENS, KV_HEADS, HEAD_DIM)
    padding = ((SPAN_RADIUS, SPAN_RADIUS), (0, 0), (0, 0))
    att_out, log_weight = window_attention(att_query.reshape(TOKENS, KV_HEADS, group, HEAD_DIM), jnp.pad(att_key, padding), jnp.pad(att_value, padding), sink.reshape(KV_HEADS, group), 0, TOKENS, min(TOK_DEV, 512))
    ret_query = project(q_ret).astype(jnp.bfloat16).reshape(TOKENS, RET_HEADS, HEAD_DIM)
    ret_key = (jnp.dot(scaled, k_ret, preferred_element_type=jnp.float32) * (inverse * HEAD_DIM ** (-0.5))).astype(jnp.bfloat16).reshape(TOKENS, RET_HEADS, HEAD_DIM)
    ret_value = project(v_ret).astype(jnp.bfloat16).reshape(TOKENS, RET_HEADS, HEAD_DIM)
    ret_out = retention(ret_query, ret_key, ret_value, decay_log)
    att_width = ATT_HEADS * HEAD_DIM // N_TP
    ret_width = RET_HEADS * HEAD_DIM // N_TP
    summed = jnp.zeros((TOKENS, D), jnp.float32)
    for member in range(N_TP):
        term = jnp.dot(att_out[:, member * att_width:(member + 1) * att_width], out_att[member * att_width:(member + 1) * att_width], preferred_element_type=jnp.float32)
        term = term + jnp.dot(ret_out[:, member * ret_width:(member + 1) * ret_width], out_ret[member * ret_width:(member + 1) * ret_width], preferred_element_type=jnp.float32)
        summed = summed + lax.optimization_barrier(term.astype(jnp.bfloat16)).astype(jnp.float32)
    return (summed.astype(jnp.bfloat16), log_weight)
```

```python
import functools

import jax
import jax.numpy as jnp
from jax import lax
from jax.experimental import pallas as pl
from jax.experimental.pallas import tpu as pltpu
from jax.sharding import Mesh
from jax.sharding import PartitionSpec as P

HEAD = 128
RADIUS = 128
CORES = 2
CHUNKS = 8
MESH = pl.DeviceIdType.MESH
BF = jnp.bfloat16
F32 = jnp.float32

NT = (((1,), (1,)), ((), ()))


def dot(a, b, dims=None):
    if dims is None:
        return jnp.dot(a, b, preferred_element_type=F32)
    return lax.dot_general(a, b, dims, preferred_element_type=F32)


def column(row, lanes):
    return jnp.broadcast_to(row, (lanes, row.shape[1])).T


def row_of(col):
    return jnp.broadcast_to(col, (col.shape[0], HEAD)).T[0:1]


def layer_kernel(
    n,
    n_tp,
    tok_ref,
    gain_ref,
    qa_ref,
    ka_ref,
    va_ref,
    qr_ref,
    kr_ref,
    vr_ref,
    oa_ref,
    or_ref,
    sink_ref,
    decay_ref,
    cos_ref,
    sin_ref,
    mixed_ref,
    logw_ref,
    w1,
    w2,
    w3,
    tok,
    ssq,
    kv,
    st1,
    r1,
    st2,
    r2,
    st3,
    r3,
    pre,
    ret,
    dmat,
    tlead,
    heads,
    pbuf,
    dbuf,
    sbuf,
    rbuf,
    ssem,
    rsem,
    tsend,
    trecv,
    qsend,
    qrecv,
    hsend,
    hrecv,
    e1send,
    e1recv,
    e2send,
    e2recv,
    e3send,
    e3recv,
    dsend,
    drecv,
    xsend,
    xrecv,
):
    nx = n_tp // CORES
    rows, width = tok_ref.shape
    model = width * n_tp
    block = qa_ref.shape[0]
    z, y, t = lax.axis_index("sp_0"), lax.axis_index("sp_1"), lax.axis_index("tp")
    x, core = lax.div(t, CORES), lax.rem(t, CORES)
    sp = z * n + y
    half = n // 2
    flip = core == 0
    a, b = jnp.where(flip, y, z), jnp.where(flip, z, y)
    step_a, step_b = jnp.where(flip, 1, n), jnp.where(flip, n, 1)

    def wrap(i, m):
        return lax.rem(i + 2 * m, m)

    def at(a_to, b_to):
        return {"sp_0": jnp.where(flip, b_to, a_to), "sp_1": jnp.where(flip, a_to, b_to)}

    def tp_of(x_to, core_to):
        return {"tp": x_to * CORES + core_to}

    def remote(src, dst, send, recv, device):
        return pltpu.make_async_remote_copy(
            src_ref=src,
            dst_ref=dst,
            send_sem=send,
            recv_sem=recv,
            device_id=device,
            device_id_type=MESH,
        )

    after = wrap(sp + 1, n * n)
    before = wrap(sp - 1, n * n)
    next_dev = {"sp_0": lax.div(after, n), "sp_1": lax.rem(after, n)}
    prev_dev = {"sp_0": lax.div(before, n), "sp_1": lax.rem(before, n)}

    barrier = pltpu.get_barrier_semaphore()
    for k in range(1, n):
        pl.semaphore_signal(barrier, 1, device_id={"sp_1": wrap(y + k, n)}, device_id_type=MESH)
        pl.semaphore_signal(barrier, 1, device_id={"sp_0": wrap(z + k, n)}, device_id_type=MESH)
    for k in range(1, n_tp):
        pl.semaphore_signal(barrier, 1, device_id={"tp": wrap(t + k, n_tp)}, device_id_type=MESH)
    pl.semaphore_signal(barrier, 1, device_id=next_dev, device_id_type=MESH)
    pl.semaphore_signal(barrier, 1, device_id=prev_dev, device_id_type=MESH)

    own = pl.ds(pl.multiple_of(sp * block, block), block)
    w1[own, 0:HEAD] = kr_ref[...]
    w1[own, HEAD : 2 * HEAD] = vr_ref[...]
    w2[own, 0:HEAD] = ka_ref[...]
    w2[own, HEAD : 2 * HEAD] = va_ref[...]
    w2[own, 2 * HEAD : 4 * HEAD] = qa_ref[...]
    w2[own, 4 * HEAD : 5 * HEAD] = qr_ref[...]
    cols = oa_ref.shape[0]
    own_out = pl.ds(pl.multiple_of(sp * cols, cols), cols)
    w3[own_out, 0 : 2 * HEAD] = oa_ref[...]
    w3[own_out, 2 * HEAD : 3 * HEAD] = or_ref[...]

    groups = ((w1, block), (w2, block), (w3, cols))

    def piece(g, a_from, b_from):
        buffer, size = groups[g]
        index = a_from * step_a + b_from * step_b
        return buffer.at[pl.ds(pl.multiple_of(index * size, size), size)], index

    def ring_copy(g, a_from, b_from, device):
        ref, index = piece(g, a_from, b_from)
        return remote(ref, ref, ssem.at[g], rsem.at[g, index], device)

    def origin(i):
        away = lax.div(i + 1, 2)
        return wrap(jnp.where(lax.rem(i, 2) == 0, a + away, a - away), n)

    b_up, b_down = wrap(b + 1, n), wrap(b - 1, n)
    a_up, a_down = wrap(a + 1, n), wrap(a - 1, n)

    def second_start(g, i, a_from):
        up = half if i < half else half - 1
        down = n - 1 - up
        if up:
            ring_copy(g, a_from, b, at(a, b_up)).start()
        if down:
            ring_copy(g, a_from, b, at(a, b_down)).start()

    def first_start(g):
        ring_copy(g, a, b, at(a_up, b)).start()
        if half > 1:
            ring_copy(g, a, b, at(a_down, b)).start()
        second_start(g, 0, a)

    def first_rest(g):
        for h in range(1, half + 1):
            a_from = wrap(a - h, n)
            ring_copy(g, a_from, b, at(a_up, b)).wait_recv()
            if h < half:
                ring_copy(g, a_from, b, at(a_up, b)).start()
            second_start(g, 2 * h - 1, a_from)
            if h < half:
                a_from = wrap(a + h, n)
                ring_copy(g, a_from, b, at(a_down, b)).wait_recv()
                if h < half - 1:
                    ring_copy(g, a_from, b, at(a_down, b)).start()
                second_start(g, 2 * h, a_from)

    def second_hop(g, h):
        def turn(i, up, down):
            a_from = origin(i)
            if up >= h:
                b_from = wrap(b - h, n)
                ring_copy(g, a_from, b_from, at(a, b_up)).wait_recv()
                if up > h:
                    ring_copy(g, a_from, b_from, at(a, b_up)).start()
            if down >= h:
                b_from = wrap(b + h, n)
                ring_copy(g, a_from, b_from, at(a, b_down)).wait_recv()
                if down > h:
                    ring_copy(g, a_from, b_from, at(a, b_down)).start()

        @pl.loop(0, half)
        def _(i):
            turn(i, half, half - 1)

        @pl.loop(half, n)
        def _(i):
            turn(i, half - 1, half)

    def ring_done(g):
        buffer, size = groups[g]
        everything = buffer.at[pl.ds(0, (n * n - 1) * size)]
        remote(everything, everything, ssem.at[g], ssem.at[g], at(a_up, b)).wait_send()

    pl.semaphore_wait(barrier, 2 * (n - 1) + (n_tp - 1) + 2)
    first_start(0)

    def token_slot(t_from):
        return pl.ds(pl.multiple_of(t_from * width, width), width)

    widened = tok_ref[...].astype(F32)
    tok[:, token_slot(t)] = (widened * gain_ref[...]).astype(BF)
    ssq[t] = jnp.broadcast_to(
        row_of(jnp.sum(widened * widened, axis=1, keepdims=True)), (8, rows)
    )

    def token_copy(k, t_from, device, part=None):
        ref = tok.at[:, token_slot(t_from)]
        if part is not None:
            ref = tok.at[pl.ds(part * (rows // 2), rows // 2), token_slot(t_from)]
        return remote(ref, ref, tsend.at[k], trecv.at[k], device)

    partner = tp_of(x, 1 - core)
    x_up, x_down, x_far = wrap(x + 1, nx), wrap(x - 1, nx), wrap(x + 2, nx)
    token_sends = []

    def send_tokens(*args):
        copy = token_copy(*args)
        copy.start()
        token_sends.append(copy)

    send_tokens(0, t, partner)
    if nx == 4:
        send_tokens(1, t, tp_of(x_up, core))
        send_tokens(2, t, tp_of(x_down, core))
    square_sends = []
    for k in range(1, n_tp):
        copy = remote(
            ssq.at[t], ssq.at[t], qsend.at[k - 1], qrecv.at[k - 1], {"tp": wrap(t + k, n_tp)}
        )
        copy.start()
        square_sends.append(copy)

    first_rest(0)
    first_start(1)

    ii = lax.broadcasted_iota(jnp.int32, (rows, rows), 0)
    jj = lax.broadcasted_iota(jnp.int32, (rows, rows), 1)
    cumul = jnp.sum(jnp.where(jj <= ii, decay_ref[...], 0.0), axis=1, keepdims=True)
    cumul_row = row_of(cumul)
    last = cumul_row[:, rows - 1 : rows]
    dmat[...] = jnp.exp(-jnp.abs(cumul - cumul_row))
    tlead[0] = jnp.broadcast_to(jnp.exp(last - cumul), (rows, HEAD))
    tlead[1] = jnp.broadcast_to(jnp.exp(cumul), (rows, HEAD))

    if nx == 4:
        from_down, from_up = x_down * CORES + core, x_up * CORES + core
        token_copy(1, from_down, partner).wait_recv()
        send_tokens(3, from_down, tp_of(x_up, core), 0)
        send_tokens(5, from_down, partner)
        token_copy(2, from_up, partner).wait_recv()
        send_tokens(4, from_up, tp_of(x_down, core), 1)
        send_tokens(6, from_up, partner)

    second_hop(0, 1)

    if nx == 4:
        from_far = x_far * CORES + core
        token_copy(3, from_far, partner, 0).wait_recv()
        token_copy(4, from_far, partner, 1).wait_recv()
        send_tokens(7, from_far, partner)

    for h in range(2, half + 1):
        second_hop(0, h)
        if h == 2:
            first_rest(1)
    if half < 2:
        first_rest(1)

    token_copy(0, x * CORES + 1 - core, partner).wait_recv()
    if nx == 4:
        for k, x_from in ((5, x_down), (6, x_up), (7, x_far)):
            token_copy(k, x_from * CORES + 1 - core, partner).wait_recv()
    for k in range(1, n_tp):
        t_from = wrap(t - k, n_tp)
        remote(
            ssq.at[t_from], ssq.at[t_from], qsend.at[k - 1], qrecv.at[k - 1], partner
        ).wait_recv()
    squares = ssq[0]
    for k in range(1, n_tp):
        squares = squares + ssq[k]
    inverse = column(lax.rsqrt(squares[0:1] / model + 1e-06), HEAD)

    first_part = dot(tok[...], w1[...])
    ret_key = (first_part[:, 0:HEAD] * (inverse * HEAD ** (-0.5))).astype(BF)
    ret_value = (first_part[:, HEAD:] * inverse).astype(BF)
    ret[0] = ret_key
    ret[1] = ret_value
    key_f = ret_key.astype(F32)
    turned = jnp.concatenate([(key_f * tlead[0]).T, (key_f * tlead[1]).T], axis=0)
    states = dot(turned.astype(BF), ret_value)
    part = HEAD // n
    st1[:, 0] = states[0:HEAD].reshape(n, part, HEAD).astype(BF)
    st1[:, 1] = states[HEAD:].reshape(n, part, HEAD).astype(BF)

    def spread(total):
        high = jnp.broadcast_to(total, (part, HEAD)).astype(BF).astype(F32)
        low = jnp.broadcast_to(total, (part, HEAD)) - high
        line = lax.broadcasted_iota(jnp.int32, (part, HEAD), 0)
        return jnp.where(line == 0, high, jnp.where(line == 1, low, 0.0)).astype(BF)

    def gathered(tile):
        return jnp.sum(tile[0:2].astype(F32), axis=0, keepdims=True)

    st1[:, 2] = jnp.broadcast_to(spread(last)[None], (n, part, HEAD))

    exchanges = []

    def exchange(k, src, dst, send, recv, device):
        copy = remote(src, dst, send.at[k - 1], recv.at[k - 1], device)
        copy.start()
        exchanges.append(copy)

    for k in range(1, n):
        y_to = wrap(y + k, n)
        exchange(k, st1.at[y_to], r1.at[y], e1send, e1recv, {"sp_1": y_to})
    r1[y] = st1[y]

    first_start(2)
    second_hop(1, 1)

    for k in range(1, n):
        y_from = wrap(y - k, n)
        remote(st1.at[y_from], r1.at[y_from], e1send.at[0], e1recv.at[k - 1], partner).wait_recv()
    logs = [gathered(r1[k, 2]) for k in range(n)]
    total = logs[0]
    for k in range(1, n):
        total = total + logs[k]
    decays = [jnp.exp(v) for v in logs]
    ahead = jnp.zeros((part, HEAD), F32)
    for k in range(n):
        pre[k, 0] = ahead
        ahead = decays[k] * ahead + r1[k, 0].astype(F32)
    behind = jnp.zeros((part, HEAD), F32)
    for k in reversed(range(n)):
        pre[k, 1] = behind
        behind = decays[k] * behind + r1[k, 1].astype(F32)
    st2[0] = ahead.astype(BF)
    st2[1] = behind.astype(BF)
    st2[2] = spread(total)
    for k in range(1, n):
        exchange(k, st2, r2.at[z], e2send, e2recv, {"sp_0": wrap(z + k, n)})

    if half >= 2:
        second_hop(1, 2)
    first_rest(2)

    for k in range(1, n):
        z_from = wrap(z - k, n)
        remote(st2, r2.at[z_from], e2send.at[0], e2recv.at[k - 1], partner).wait_recv()
    r2[z] = st2[...]
    ahead = jnp.zeros((part, HEAD), F32)
    for k in range(n - 1):
        moved = jnp.exp(gathered(r2[k, 2])) * ahead + r2[k, 0].astype(F32)
        ahead = jnp.where(k < z, moved, ahead)
    behind = jnp.zeros((part, HEAD), F32)
    for k in reversed(range(1, n)):
        moved = jnp.exp(gathered(r2[k, 2])) * behind + r2[k, 1].astype(F32)
        behind = jnp.where(k > z, moved, behind)
    for k in range(n):
        st3[k, 0] = (pre[k, 0] + ahead).astype(BF)
        ahead = ahead * decays[k]
    for k in reversed(range(n)):
        st3[k, 1] = (pre[k, 1] + behind).astype(BF)
        behind = behind * decays[k]
    for k in range(1, n):
        y_to = wrap(y + k, n)
        exchange(k, st3.at[y_to], r3.at[y], e3send, e3recv, {"sp_1": y_to})

    for h in range(3, half + 1):
        second_hop(1, h)

    second_part = dot(tok[...], w2[...])
    cosine, sine = cos_ref[...], sin_ref[...]

    def rotated(v):
        return v * cosine + pltpu.roll(v, HEAD // 2, 1) * sine

    def taken(k):
        return second_part[:, k * HEAD : (k + 1) * HEAD] * inverse

    kv[0, RADIUS : RADIUS + rows] = rotated(taken(0)).astype(BF)
    kv[1, RADIUS : RADIUS + rows] = taken(1).astype(BF)
    to_next = remote(
        kv.at[:, pl.ds(rows, RADIUS)],
        kv.at[:, pl.ds(0, RADIUS)],
        hsend.at[0],
        hrecv.at[0],
        next_dev,
    )
    to_prev = remote(
        kv.at[:, pl.ds(RADIUS, RADIUS)],
        kv.at[:, pl.ds(RADIUS + rows, RADIUS)],
        hsend.at[1],
        hrecv.at[1],
        prev_dev,
    )
    to_next.start()
    to_prev.start()
    queries = [rotated(taken(2 + k)).astype(BF) for k in range(2)]
    ret[3] = queries[0]
    ret[4] = queries[1]
    ret[2] = taken(4).astype(BF)

    second_hop(2, 1)

    for k in range(1, n):
        y_from = wrap(y - k, n)
        remote(st3.at[y_from], r3.at[y_from], e3send.at[0], e3recv.at[k - 1], partner).wait_recv()
    r3[y] = st3[y]
    ret_query = ret[2]
    weights = (dot(ret_query, ret[0], NT) * dmat[...]).astype(BF)
    mix = dot(weights, ret[1])
    mix = mix + tlead[1] * dot(ret_query, r3[:, 0].reshape(HEAD, HEAD))
    mix = mix + tlead[0] * dot(ret_query, r3[:, 1].reshape(HEAD, HEAD))
    middle = mix - jnp.mean(mix, axis=1, keepdims=True)
    normed = middle * lax.rsqrt(jnp.mean(middle * middle, axis=1, keepdims=True) + 1e-06)
    heads[:, 2 * HEAD :] = normed.astype(BF)

    if half >= 2:
        second_hop(2, 2)

    to_next.wait_recv()
    to_prev.wait_recv()
    span = rows + 2 * RADIUS
    query_at = lax.broadcasted_iota(jnp.int32, (rows, span), 0)
    key_at = lax.broadcasted_iota(jnp.int32, (rows, span), 1) - RADIUS
    key_pos = key_at + sp * rows
    valid = (
        (jnp.abs(key_at - query_at) <= RADIUS) & (key_pos >= 0) & (key_pos < n * n * rows)
    )
    for k in range(2):
        scores = dot(ret[3 + k], kv[0], NT) * HEAD ** (-0.5)
        masked = jnp.where(valid, scores, -jnp.inf)
        sink = sink_ref[k]
        top = jnp.maximum(jnp.max(masked, axis=1, keepdims=True), sink)
        expo = jnp.exp(masked - top)
        total = jnp.sum(expo, axis=1, keepdims=True) + jnp.exp(sink - top)
        logw_ref[k : k + 1, :] = row_of(top + jnp.log(total))
        probs = (expo * (1.0 / total)).astype(BF)
        heads[:, k * HEAD : (k + 1) * HEAD] = dot(probs, kv[1]).astype(BF)

    for h in range(3, half + 1):
        second_hop(2, h)

    size = model // CHUNKS
    mine = rows // n_tp

    def core_copy(c):
        return remote(pbuf.at[c, 1 - core], dbuf.at[c], dsend.at[c], drecv.at[c], partner)

    def x_copy(c, k):
        x_to = wrap(x + k, nx)
        return remote(
            sbuf.at[c, x_to],
            rbuf.at[c, k - 1],
            xsend.at[c, k - 1],
            xrecv.at[c, k - 1],
            tp_of(x_to, core),
        )

    @pl.loop(0, CHUNKS + 2)
    def _(c):
        @pl.when(c < CHUNKS)
        def _():
            partial = dot(heads[...], w3[pl.ds(pl.multiple_of(c * size, size), size)], NT)
            parted = partial.astype(BF).reshape(nx, CORES, mine, size)
            for k in range(CORES):
                pbuf[c, k] = parted[:, k]
            core_copy(c).start()

        @pl.when((c >= 1) & (c < CHUNKS + 1))
        def _():
            d = c - 1
            core_copy(d).wait_recv()
            sbuf[d] = (pbuf[d, core].astype(F32) + dbuf[d].astype(F32)).astype(BF)
            for k in range(1, nx):
                x_copy(d, k).start()

        @pl.when(c >= 2)
        def _():
            d = c - 2
            result = sbuf[d, x].astype(F32)
            for k in range(1, nx):
                x_copy(d, k).wait_recv()
                result = result + rbuf[d, k - 1].astype(F32)
            mixed_ref[:, pl.ds(pl.multiple_of(d * size, size), size)] = result.astype(BF)

    for g in range(3):
        ring_done(g)
    for copy in token_sends + square_sends + exchanges:
        copy.wait_send()
    to_next.wait_send()
    to_prev.wait_send()

    @pl.loop(0, CHUNKS)
    def _(c):
        core_copy(c).wait_send()
        for k in range(1, nx):
            x_copy(c, k).wait_send()


def layer(n, n_tp, *args):
    tokens, gain, qa, ka, va, qr, kr, vr, oa, orr, sink, decay = args
    rows, width = tokens.shape
    model = width * n_tp
    offset = (lax.axis_index("sp_0") * n + lax.axis_index("sp_1")) * rows
    positions = (offset + jnp.arange(rows, dtype=jnp.int32)).astype(F32)
    freqs = 10000.0 ** (-jnp.arange(0, HEAD, 2).astype(F32) / HEAD)
    angles = positions[:, None] * freqs[None, :]
    cosine, sine = jnp.cos(angles), jnp.sin(angles)
    cosine = jnp.concatenate([cosine, cosine], axis=1)
    sine = jnp.concatenate([-sine, sine], axis=1)
    nx = n_tp // CORES
    part = HEAD // n
    size = model // CHUNKS
    mine = rows // n_tp
    vmem = pl.BlockSpec(memory_space=pltpu.VMEM)
    dma = pltpu.SemaphoreType.DMA
    return pl.pallas_call(
        functools.partial(layer_kernel, n, n_tp),
        name="layer",
        out_shape=(
            jax.ShapeDtypeStruct((mine, model), BF),
            jax.ShapeDtypeStruct((2, rows), F32),
        ),
        in_specs=[vmem] * 10 + [pl.BlockSpec(memory_space=pltpu.SMEM)] + [vmem] * 3,
        out_specs=(vmem, vmem),
        scratch_shapes=[
            pltpu.VMEM((model, 2 * HEAD), BF),
            pltpu.VMEM((model, 5 * HEAD), BF),
            pltpu.VMEM((model, 3 * HEAD), BF),
            pltpu.VMEM((rows, model), BF),
            pltpu.VMEM((n_tp, 8, rows), F32),
            pltpu.VMEM((2, rows + 2 * RADIUS, HEAD), BF),
            pltpu.VMEM((n, 3, part, HEAD), BF),
            pltpu.VMEM((n, 3, part, HEAD), BF),
            pltpu.VMEM((3, part, HEAD), BF),
            pltpu.VMEM((n, 3, part, HEAD), BF),
            pltpu.VMEM((n, 2, part, HEAD), BF),
            pltpu.VMEM((n, 2, part, HEAD), BF),
            pltpu.VMEM((n, 2, part, HEAD), F32),
            pltpu.VMEM((5, rows, HEAD), BF),
            pltpu.VMEM((rows, rows), F32),
            pltpu.VMEM((2, rows, HEAD), F32),
            pltpu.VMEM((rows, 3 * HEAD), BF),
            pltpu.VMEM((CHUNKS, CORES, nx, mine, size), BF),
            pltpu.VMEM((CHUNKS, nx, mine, size), BF),
            pltpu.VMEM((CHUNKS, nx, mine, size), BF),
            pltpu.VMEM((CHUNKS, max(nx - 1, 1), mine, size), BF),
            dma((3,)),
            dma((3, n * n)),
            dma((8,)),
            dma((8,)),
            dma((n_tp - 1,)),
            dma((n_tp - 1,)),
            dma((2,)),
            dma((2,)),
            dma((n - 1,)),
            dma((n - 1,)),
            dma((n - 1,)),
            dma((n - 1,)),
            dma((n - 1,)),
            dma((n - 1,)),
            dma((CHUNKS,)),
            dma((CHUNKS,)),
            dma((CHUNKS, max(nx - 1, 1))),
            dma((CHUNKS, max(nx - 1, 1))),
        ],
        compiler_params=pltpu.CompilerParams(
            collective_id=0, has_side_effects=True, vmem_limit_bytes=56 * 1024 * 1024
        ),
    )(
                tokens,
        gain.reshape(1, width),
        qa,
        ka,
        va,
        qr,
        kr,
        vr,
        oa.T,
        orr.T,
        sink,
        decay,
        cosine,
        sine,
    )


SP = ("sp_0", "sp_1")


def solution(mesh):
    n_tp = mesh.shape["tp"]
    n = round(mesh.shape["sp"] ** 0.5)
    finer = Mesh(mesh.devices.reshape(n, n, n_tp), ("sp_0", "sp_1", "tp"))
    return jax.shard_map(
        functools.partial(layer, n, n_tp),
        mesh=finer,
        in_specs=(
            P(SP, "tp"),
            P("tp"),
            P(SP, "tp"),
            P(SP, "tp"),
            P(SP, "tp"),
            P(SP, "tp"),
            P(SP, "tp"),
            P(SP, "tp"),
            P("tp", SP),
            P("tp", SP),
            P("tp"),
            P("tp", SP),
        ),
        out_specs=(P(("sp_0", "sp_1", "tp"), None), P("tp", SP)),
        check_vma=False,
    )
```

```python
import functools

import jax
import jax.numpy as jnp
from jax import lax
from jax.experimental import pallas as pl
from jax.experimental.pallas import tpu as pltpu
from jax.sharding import Mesh
from jax.sharding import PartitionSpec as P

HEAD = 128
RADIUS = 128
CORES = 2
MESH = pl.DeviceIdType.MESH
BF = jnp.bfloat16
F32 = jnp.float32

NT = (((1,), (1,)), ((), ()))

(
    PEERS, FIRST, SET_OUT, HOP, TOKENS_OUT, TOKENS_ON, TOKENS_FAR, TOKENS_IN, DECAYS,
    ANGLES, STATES, ALONG_Y, ALONG_Z, PROJECT_KEYS, PROJECT_QUERIES, PROJECT_RETENTION,
    RETENTION, ATTENTION, PARTIAL_SUMS, CORE_SUMS, X_SUMS, LAST_SUMS, DRAIN,
) = range(23)
ORDER = (
    (PEERS,), (FIRST, 0, 0), (SET_OUT, 0, 0), (FIRST, 1, 0), (SET_OUT, 1, 0), (FIRST, 2, 0),
    (TOKENS_OUT,), (DECAYS,), (ANGLES,), (FIRST, 0, 1), (SET_OUT, 0, 1), (HOP, 0, 1, 0),
    (FIRST, 1, 1), (SET_OUT, 1, 1), (FIRST, 2, 1), (HOP, 1, 1, 0), (FIRST, 0, 2),
    (SET_OUT, 0, 2), (TOKENS_ON,), (HOP, 0, 1, 1), (HOP, 0, 2, 0), (FIRST, 1, 2),
    (SET_OUT, 1, 2), (HOP, 1, 1, 1), (FIRST, 2, 2), (FIRST, 0, 3), (SET_OUT, 0, 3),
    (HOP, 0, 1, 2), (HOP, 0, 2, 1), (HOP, 0, 3, 0), (FIRST, 1, 3), (SET_OUT, 1, 3),
    (HOP, 1, 1, 2), (FIRST, 0, 4), (SET_OUT, 0, 4), (FIRST, 2, 3), (HOP, 1, 2, 0),
    (HOP, 0, 1, 3), (HOP, 0, 2, 2), (HOP, 0, 3, 1), (HOP, 0, 4, 0), (FIRST, 1, 4),
    (SET_OUT, 1, 4), (TOKENS_FAR,), (HOP, 1, 1, 3), (HOP, 1, 2, 1), (FIRST, 2, 4),
    (HOP, 1, 2, 2), (HOP, 0, 1, 4), (HOP, 0, 2, 3), (HOP, 0, 3, 2), (HOP, 0, 4, 1),
    (HOP, 1, 1, 4), (HOP, 1, 2, 3), (HOP, 1, 3, 0), (HOP, 0, 2, 4), (HOP, 0, 3, 3),
    (HOP, 0, 4, 2), (HOP, 1, 2, 4), (HOP, 1, 3, 1), (SET_OUT, 2, 0), (SET_OUT, 2, 1),
    (HOP, 0, 3, 4), (HOP, 0, 4, 3), (SET_OUT, 2, 2), (HOP, 1, 3, 2), (SET_OUT, 2, 3),
    (SET_OUT, 2, 4), (HOP, 1, 3, 3), (HOP, 1, 3, 4), (HOP, 0, 4, 4), (TOKENS_IN,), (STATES,),
    (HOP, 1, 4, 0), (HOP, 1, 4, 1), (HOP, 2, 1, 0), (HOP, 2, 1, 1), (HOP, 1, 4, 2),
    (HOP, 2, 1, 2), (HOP, 1, 4, 3), (HOP, 2, 1, 3), (HOP, 2, 1, 4), (ALONG_Y,), (HOP, 1, 4, 4),
    (PROJECT_KEYS,), (HOP, 2, 2, 0), (HOP, 2, 2, 1), (PROJECT_QUERIES,), (HOP, 2, 2, 2),
    (HOP, 2, 2, 3), (HOP, 2, 2, 4), (PROJECT_RETENTION,), (HOP, 2, 3, 0), (HOP, 2, 3, 1),
    (ATTENTION, 0), (ALONG_Z,), (HOP, 2, 3, 2), (ATTENTION, 1), (HOP, 2, 3, 3), (HOP, 2, 3, 4),
    (HOP, 2, 4, 0), (HOP, 2, 4, 1), (HOP, 2, 4, 2), (HOP, 2, 4, 3), (HOP, 2, 4, 4),
    (RETENTION,), (PARTIAL_SUMS, 0), (PARTIAL_SUMS, 1), (CORE_SUMS, 0), (PARTIAL_SUMS, 2),
    (CORE_SUMS, 1), (PARTIAL_SUMS, 3), (CORE_SUMS, 2), (PARTIAL_SUMS, 4), (CORE_SUMS, 3),
    (PARTIAL_SUMS, 5), (CORE_SUMS, 4), (PARTIAL_SUMS, 6), (CORE_SUMS, 5), (PARTIAL_SUMS, 7),
    (X_SUMS, 0), (CORE_SUMS, 6), (X_SUMS, 1), (CORE_SUMS, 7), (X_SUMS, 2), (X_SUMS, 3),
    (X_SUMS, 4), (X_SUMS, 5), (X_SUMS, 6), (X_SUMS, 7), (LAST_SUMS, 0), (LAST_SUMS, 1),
    (LAST_SUMS, 2), (LAST_SUMS, 3), (LAST_SUMS, 4), (LAST_SUMS, 5), (LAST_SUMS, 6),
    (LAST_SUMS, 7), (DRAIN,),
)


def dot(a, b, dims=None):
    if dims is None:
        return jnp.dot(a, b, preferred_element_type=F32)
    return lax.dot_general(a, b, dims, preferred_element_type=F32)


def column(row, lanes):
    return jnp.broadcast_to(row, (lanes, row.shape[1])).T


def row_of(col):
    return jnp.broadcast_to(col, (col.shape[0], HEAD)).T[0:1]


def layer_kernel(
    n,
    n_tp,
    tok_ref,
    gain_ref,
    qa_ref,
    ka_ref,
    va_ref,
    qr_ref,
    kr_ref,
    vr_ref,
    oa_ref,
    or_ref,
    sink_ref,
    decay_ref,
    freq_ref,
    mixed_ref,
    logw_ref,
    w1,
    w2,
    w3,
    tok,
    ssq,
    kv,
    st1,
    r1,
    st2,
    r2,
    st3,
    r3,
    pre,
    ret,
    dmat,
    tlead,
    inv,
    turns,
    heads,
    pbuf,
    dbuf,
    sbuf,
    rbuf,
    ssem,
    rsem,
    tsend,
    trecv,
    qsend,
    qrecv,
    hsend,
    hrecv,
    e1send,
    e1recv,
    e2send,
    e2recv,
    e3send,
    e3recv,
    dsend,
    drecv,
    xsend,
    xrecv,
):
    nx = n_tp // CORES
    rows, width = tok_ref.shape
    model = width * n_tp
    block = qa_ref.shape[0]
    z, y, t = lax.axis_index("sp_0"), lax.axis_index("sp_1"), lax.axis_index("tp")
    x, core = lax.div(t, CORES), lax.rem(t, CORES)
    sp = z * n + y
    half = n // 2
    flip = core == 0

    def wrap(i, m):
        return lax.rem(i + 2 * m, m)

    def place(g):
        return jnp.where(flip, y, z), jnp.where(flip, z, y)

    def at(g, a_to, b_to):
        return {"sp_0": jnp.where(flip, b_to, a_to), "sp_1": jnp.where(flip, a_to, b_to)}

    def tp_of(x_to, core_to):
        return {"tp": x_to * CORES + core_to}

    def remote(src, dst, send, recv, device):
        return pltpu.make_async_remote_copy(
            src_ref=src,
            dst_ref=dst,
            send_sem=send,
            recv_sem=recv,
            device_id=device,
            device_id_type=MESH,
        )

    partner = tp_of(x, 1 - core)
    after = wrap(sp + 1, n * n)
    before = wrap(sp - 1, n * n)
    next_dev = {"sp_0": lax.div(after, n), "sp_1": lax.rem(after, n)}
    prev_dev = {"sp_0": lax.div(before, n), "sp_1": lax.rem(before, n)}

    barrier = pltpu.get_barrier_semaphore()
    for k in range(1, n):
        pl.semaphore_signal(barrier, 1, device_id={"sp_1": wrap(y + k, n)}, device_id_type=MESH)
        pl.semaphore_signal(barrier, 1, device_id={"sp_0": wrap(z + k, n)}, device_id_type=MESH)
    for k in range(1, n_tp):
        pl.semaphore_signal(barrier, 1, device_id={"tp": wrap(t + k, n_tp)}, device_id_type=MESH)
    pl.semaphore_signal(barrier, 1, device_id=next_dev, device_id_type=MESH)
    pl.semaphore_signal(barrier, 1, device_id=prev_dev, device_id_type=MESH)

    own = pl.ds(pl.multiple_of(sp * block, block), block)
    w1[own, 0:HEAD] = kr_ref[...]
    w1[own, HEAD : 2 * HEAD] = vr_ref[...]
    w2[own, 0:HEAD] = ka_ref[...]
    w2[own, HEAD : 2 * HEAD] = va_ref[...]
    w2[own, 2 * HEAD : 4 * HEAD] = qa_ref[...]
    w2[own, 4 * HEAD : 5 * HEAD] = qr_ref[...]
    cols = oa_ref.shape[0]
    own_out = pl.ds(pl.multiple_of(sp * cols, cols), cols)
    w3[own_out, 0 : 2 * HEAD] = oa_ref[...]
    w3[own_out, 2 * HEAD : 3 * HEAD] = or_ref[...]

    groups = ((w1, block), (w2, block), (w3, cols))

    def ring_copy(g, a_from, b_from, device=None):
        buffer, size = groups[g]
        index = jnp.where(flip, b_from * n + a_from, a_from * n + b_from)
        ref = buffer.at[pl.ds(pl.multiple_of(index * size, size), size)]
        return remote(ref, ref, ssem.at[g], rsem.at[g, index], device or at(g, *place(g)))

    def steps(g, k):
        a, _ = place(g)
        if k == 0:
            return [(0, a)]
        if k > half:
            return []
        up = [(2 * k - 1, wrap(a - k, n))]
        return up + [(2 * k, wrap(a + k, n))] if k < half else up

    def first(g, k):
        a, b = place(g)
        up, down = at(g, wrap(a + 1, n), b), at(g, wrap(a - 1, n), b)
        if k == 0:
            ring_copy(g, a, b, up).start()
            if half > 1:
                ring_copy(g, a, b, down).start()
            return
        if k > half:
            return
        a_from = wrap(a - k, n)
        ring_copy(g, a_from, b).wait_recv()
        if k < half:
            ring_copy(g, a_from, b, up).start()
            a_from = wrap(a + k, n)
            ring_copy(g, a_from, b).wait_recv()
            if k < half - 1:
                ring_copy(g, a_from, b, down).start()

    def set_out(g, k):
        hop(g, 0, k)

    def hop(g, h, k):
        a, b = place(g)
        if h > half:
            return
        for i, a_from in steps(g, k):
            hops_up = half if i < half else half - 1
            for hops, way in ((hops_up, 1), (n - 1 - hops_up, -1)):
                if hops >= h:
                    b_from = wrap(b - way * h, n)
                    if h > 0:
                        ring_copy(g, a_from, b_from).wait_recv()
                    if hops > h:
                        there = at(g, a, wrap(b + way, n))
                        ring_copy(g, a_from, b_from, there).start()

    def ring_done(g):
        buffer, size = groups[g]
        everything = buffer.at[pl.ds(0, (n * n - 1) * size)]
        remote(everything, everything, ssem.at[g], ssem.at[g], partner).wait_send()

    def wait_peers():
        pl.semaphore_wait(barrier, 2 * (n - 1) + (n_tp - 1) + 2)

    sent = []

    def send(copy):
        copy.start()
        sent.append(copy)

    def token_slot(t_from):
        return pl.ds(pl.multiple_of(t_from * width, width), width)

    def token_copy(k, t_from, device, part=None):
        ref = tok.at[:, token_slot(t_from)]
        if part is not None:
            ref = tok.at[pl.ds(part * (rows // 2), rows // 2), token_slot(t_from)]
        return remote(ref, ref, tsend.at[k], trecv.at[k], device)

    x_up, x_down, x_far = wrap(x + 1, nx), wrap(x - 1, nx), wrap(x + 2, nx)

    def tokens_out():
        widened = tok_ref[...].astype(F32)
        tok[:, token_slot(t)] = (widened * gain_ref[...]).astype(BF)
        ssq[t] = jnp.broadcast_to(
            row_of(jnp.sum(widened * widened, axis=1, keepdims=True)), (8, rows)
        )
        send(token_copy(0, t, partner))
        if nx == 4:
            send(token_copy(1, t, tp_of(x_up, core)))
            send(token_copy(2, t, tp_of(x_down, core)))
        for k in range(1, n_tp):
            there = {"tp": wrap(t + k, n_tp)}
            send(remote(ssq.at[t], ssq.at[t], qsend.at[k - 1], qrecv.at[k - 1], there))

    def tokens_on():
        if nx == 4:
            from_down, from_up = x_down * CORES + core, x_up * CORES + core
            token_copy(1, from_down, partner).wait_recv()
            send(token_copy(3, from_down, tp_of(x_up, core), 0))
            send(token_copy(5, from_down, partner))
            token_copy(2, from_up, partner).wait_recv()
            send(token_copy(4, from_up, tp_of(x_down, core), 1))
            send(token_copy(6, from_up, partner))

    def tokens_far():
        if nx == 4:
            from_far = x_far * CORES + core
            token_copy(3, from_far, partner, 0).wait_recv()
            token_copy(4, from_far, partner, 1).wait_recv()
            send(token_copy(7, from_far, partner))

    def tokens_in():
        token_copy(0, x * CORES + 1 - core, partner).wait_recv()
        if nx == 4:
            for k, x_from in ((5, x_down), (6, x_up), (7, x_far)):
                token_copy(k, x_from * CORES + 1 - core, partner).wait_recv()
        for k in range(1, n_tp):
            t_from = wrap(t - k, n_tp)
            remote(
                ssq.at[t_from], ssq.at[t_from], qsend.at[k - 1], qrecv.at[k - 1], partner
            ).wait_recv()
        squares = ssq[0]
        for k in range(1, n_tp):
            squares = squares + ssq[k]
        inv[...] = column(lax.rsqrt(squares[0:1] / model + 1e-06), HEAD)

    def decays():
        ii = lax.broadcasted_iota(jnp.int32, (rows, rows), 0)
        jj = lax.broadcasted_iota(jnp.int32, (rows, rows), 1)
        cumul = jnp.sum(jnp.where(jj <= ii, decay_ref[...], 0.0), axis=1, keepdims=True)
        cumul_row = row_of(cumul)
        last = cumul_row[:, rows - 1 : rows]
        dmat[...] = jnp.exp(-jnp.abs(cumul - cumul_row))
        tlead[0] = jnp.broadcast_to(jnp.exp(last - cumul), (rows, HEAD))
        tlead[1] = jnp.broadcast_to(jnp.exp(cumul), (rows, HEAD))
        st1[:, 2] = jnp.broadcast_to(spread(last)[None], (n, part, HEAD))

    part = HEAD // n

    def spread(total):
        high = jnp.broadcast_to(total, (part, HEAD)).astype(BF).astype(F32)
        low = jnp.broadcast_to(total, (part, HEAD)) - high
        line = lax.broadcasted_iota(jnp.int32, (part, HEAD), 0)
        return jnp.where(line == 0, high, jnp.where(line == 1, low, 0.0)).astype(BF)

    def gathered(tile):
        return jnp.sum(tile[0:2].astype(F32), axis=0, keepdims=True)

    def states():
        first_part = dot(tok[...], w1[...])
        inverse = inv[...]
        ret_key = (first_part[:, 0:HEAD] * (inverse * HEAD ** (-0.5))).astype(BF)
        ret_value = (first_part[:, HEAD:] * inverse).astype(BF)
        ret[0] = ret_key
        ret[1] = ret_value
        key_f = ret_key.astype(F32)
        turned = jnp.concatenate([(key_f * tlead[0]).T, (key_f * tlead[1]).T], axis=0)
        both = dot(turned.astype(BF), ret_value)
        st1[:, 0] = both[0:HEAD].reshape(n, part, HEAD).astype(BF)
        st1[:, 1] = both[HEAD:].reshape(n, part, HEAD).astype(BF)
        for k in range(1, n):
            y_to = wrap(y + k, n)
            there = {"sp_1": y_to}
            send(remote(st1.at[y_to], r1.at[y], e1send.at[k - 1], e1recv.at[k - 1], there))
        r1[y] = st1[y]

    def along_y():
        for k in range(1, n):
            y_from = wrap(y - k, n)
            remote(
                st1.at[y_from], r1.at[y_from], e1send.at[0], e1recv.at[k - 1], partner
            ).wait_recv()
        logs = [gathered(r1[k, 2]) for k in range(n)]
        total = logs[0]
        for k in range(1, n):
            total = total + logs[k]
        fades = [jnp.exp(v) for v in logs]
        ahead = jnp.zeros((part, HEAD), F32)
        for k in range(n):
            pre[k, 0] = ahead
            ahead = fades[k] * ahead + r1[k, 0].astype(F32)
        behind = jnp.zeros((part, HEAD), F32)
        for k in reversed(range(n)):
            pre[k, 1] = behind
            behind = fades[k] * behind + r1[k, 1].astype(F32)
        st2[0] = ahead.astype(BF)
        st2[1] = behind.astype(BF)
        st2[2] = spread(total)
        for k in range(1, n):
            there = {"sp_0": wrap(z + k, n)}
            send(remote(st2, r2.at[z], e2send.at[k - 1], e2recv.at[k - 1], there))

    def along_z():
        for k in range(1, n):
            z_from = wrap(z - k, n)
            remote(st2, r2.at[z_from], e2send.at[0], e2recv.at[k - 1], partner).wait_recv()
        r2[z] = st2[...]
        fades = [jnp.exp(gathered(r1[k, 2])) for k in range(n)]
        ahead = jnp.zeros((part, HEAD), F32)
        for k in range(n - 1):
            moved = jnp.exp(gathered(r2[k, 2])) * ahead + r2[k, 0].astype(F32)
            ahead = jnp.where(k < z, moved, ahead)
        behind = jnp.zeros((part, HEAD), F32)
        for k in reversed(range(1, n)):
            moved = jnp.exp(gathered(r2[k, 2])) * behind + r2[k, 1].astype(F32)
            behind = jnp.where(k > z, moved, behind)
        for k in range(n):
            st3[k, 0] = (pre[k, 0] + ahead).astype(BF)
            ahead = ahead * fades[k]
        for k in reversed(range(n)):
            st3[k, 1] = (pre[k, 1] + behind).astype(BF)
            behind = behind * fades[k]
        for k in range(1, n):
            y_to = wrap(y + k, n)
            there = {"sp_1": y_to}
            send(remote(st3.at[y_to], r3.at[y], e3send.at[k - 1], e3recv.at[k - 1], there))
        r3[y] = st3[y]

    to_next = remote(
        kv.at[:, pl.ds(rows, RADIUS)],
        kv.at[:, pl.ds(0, RADIUS)],
        hsend.at[0],
        hrecv.at[0],
        next_dev,
    )
    to_prev = remote(
        kv.at[:, pl.ds(RADIUS, RADIUS)],
        kv.at[:, pl.ds(RADIUS + rows, RADIUS)],
        hsend.at[1],
        hrecv.at[1],
        prev_dev,
    )

    def rotated(v):
        return v * turns[0] + pltpu.roll(v, HEAD // 2, 1) * turns[1]

    def angles():
        position = lax.broadcasted_iota(jnp.int32, (rows, HEAD), 0) + sp * rows
        angle = position.astype(F32) * freq_ref[...]
        second_half = lax.broadcasted_iota(jnp.int32, (rows, HEAD), 1) >= HEAD // 2
        sine = jnp.sin(angle)
        turns[0] = jnp.cos(angle)
        turns[1] = jnp.where(second_half, sine, -sine)

    def project_keys():
        both = dot(tok[...], w2[:, 0 : 2 * HEAD])
        kv[0, RADIUS : RADIUS + rows] = rotated(both[:, :HEAD] * inv[...]).astype(BF)
        kv[1, RADIUS : RADIUS + rows] = (both[:, HEAD:] * inv[...]).astype(BF)
        send(to_next)
        send(to_prev)

    def project_queries():
        both = dot(tok[...], w2[:, 2 * HEAD : 4 * HEAD])
        for k in range(2):
            own_head = both[:, k * HEAD : (k + 1) * HEAD]
            ret[3 + k] = rotated(own_head * inv[...]).astype(BF)

    def project_retention():
        ret[2] = (dot(tok[...], w2[:, 4 * HEAD :]) * inv[...]).astype(BF)

    def retention():
        for k in range(1, n):
            y_from = wrap(y - k, n)
            remote(
                st3.at[y_from], r3.at[y_from], e3send.at[0], e3recv.at[k - 1], partner
            ).wait_recv()
        ret_query = ret[2]
        weights = (dot(ret_query, ret[0], NT) * dmat[...]).astype(BF)
        mix = dot(weights, ret[1])
        mix = mix + tlead[1] * dot(ret_query, r3[:, 0].reshape(HEAD, HEAD))
        mix = mix + tlead[0] * dot(ret_query, r3[:, 1].reshape(HEAD, HEAD))
        middle = mix - jnp.mean(mix, axis=1, keepdims=True)
        normed = middle * lax.rsqrt(jnp.mean(middle * middle, axis=1, keepdims=True) + 1e-06)
        heads[:, 2 * HEAD :] = normed.astype(BF)

    def attention(k):
        if k == 0:
            to_next.wait_recv()
            to_prev.wait_recv()
        span = rows + 2 * RADIUS
        query_at = lax.broadcasted_iota(jnp.int32, (rows, span), 0)
        key_at = lax.broadcasted_iota(jnp.int32, (rows, span), 1) - RADIUS
        key_pos = key_at + sp * rows
        valid = (
            (jnp.abs(key_at - query_at) <= RADIUS) & (key_pos >= 0) & (key_pos < n * n * rows)
        )
        scores = dot(ret[3 + k], kv[0], NT) * HEAD ** (-0.5)
        masked = jnp.where(valid, scores, -jnp.inf)
        sink = sink_ref[k]
        top = jnp.maximum(jnp.max(masked, axis=1, keepdims=True), sink)
        expo = jnp.exp(masked - top)
        total = jnp.sum(expo, axis=1, keepdims=True) + jnp.exp(sink - top)
        logw_ref[k : k + 1, :] = row_of(top + jnp.log(total))
        probs = (expo * (1.0 / total)).astype(BF)
        heads[:, k * HEAD : (k + 1) * HEAD] = dot(probs, kv[1]).astype(BF)

    size = model // n
    mine = rows // n_tp
    left, right = pl.ds(0, size // 2), pl.ds(size // 2, size // 2)

    def core_copy(c):
        return remote(pbuf.at[c, 1 - core], dbuf.at[c], dsend.at[c], drecv.at[c], partner)

    def x_copy(c, k):
        up = k in (0, 2, 4)
        x_to = (x_far, x_far, x_up, x_down, x_up, x_down)[k]
        columns = (left, right, left, right, right, left)[k]
        return remote(
            sbuf.at[c, x_to, :, columns],
            rbuf.at[c, k // 2, :, left if up else right]
            if k < 2
            else rbuf.at[c, 1 if up else 2, :, columns],
            xsend.at[c, k],
            xrecv.at[c, k],
            tp_of(x_up if up else x_down, core),
        )

    def columns_of(c):
        return pl.ds(c * size, size)

    def partial_sums(c):
        if c >= n:
            return
        partial = dot(heads[...], w3[columns_of(c)], NT)
        parted = partial.astype(BF).reshape(nx, CORES, mine, size)
        for k in range(CORES):
            pbuf[c, k] = parted[:, k]
        send(core_copy(c))

    def core_sums(c):
        if c >= n:
            return
        core_copy(c).wait_recv()
        sbuf[c] = (pbuf[c, core].astype(F32) + dbuf[c].astype(F32)).astype(BF)
        if nx == 4:
            for k in (0, 1, 4, 5) if c < n // 2 else (0, 1):
                send(x_copy(c, k))

    def x_sums(c):
        if nx == 4 and c < n:
            x_copy(c, 0).wait_recv()
            passed = rbuf[c, 0, :, 0 : size // 2].astype(F32)
            sbuf[c, x_up, :, 0 : size // 2] = (
                sbuf[c, x_up, :, 0 : size // 2].astype(F32) + passed
            ).astype(BF)
            send(x_copy(c, 2))
            x_copy(c, 1).wait_recv()
            passed = rbuf[c, 0, :, size // 2 :].astype(F32)
            sbuf[c, x_down, :, size // 2 :] = (
                sbuf[c, x_down, :, size // 2 :].astype(F32) + passed
            ).astype(BF)
            send(x_copy(c, 3))
            if c >= n // 2:
                send(x_copy(c, 4))
                send(x_copy(c, 5))

    def last_sums(c):
        if c >= n:
            return
        result = sbuf[c, x].astype(F32)
        if nx == 4:
            for k in (2, 3, 4, 5):
                x_copy(c, k).wait_recv()
            result = result + rbuf[c, 1].astype(F32) + rbuf[c, 2].astype(F32)
        mixed_ref[:, columns_of(c)] = result.astype(BF)

    def drain():
        for g in range(3):
            ring_done(g)
        for copy in sent:
            copy.wait_send()

    stages = (
        wait_peers,
        first,
        set_out,
        hop,
        tokens_out,
        tokens_on,
        tokens_far,
        tokens_in,
        decays,
        angles,
        states,
        along_y,
        along_z,
        project_keys,
        project_queries,
        project_retention,
        retention,
        attention,
        partial_sums,
        core_sums,
        x_sums,
        last_sums,
        drain,
    )
    for code, *numbers in ORDER:
        stages[code](*numbers)


def layer(n, n_tp, *args):
    tokens, gain, qa, ka, va, qr, kr, vr, oa, orr, sink, decay = args
    rows, width = tokens.shape
    model = width * n_tp
    freqs = 10000.0 ** (-jnp.arange(0, HEAD, 2).astype(F32) / HEAD)
    freqs = jnp.concatenate([freqs, freqs]).reshape(1, HEAD)
    nx = n_tp // CORES
    part = HEAD // n
    size = model // n
    mine = rows // n_tp
    vmem = pl.BlockSpec(memory_space=pltpu.VMEM)
    dma = pltpu.SemaphoreType.DMA
    return pl.pallas_call(
        functools.partial(layer_kernel, n, n_tp),
        name="layer",
        out_shape=(
            jax.ShapeDtypeStruct((mine, model), BF),
            jax.ShapeDtypeStruct((2, rows), F32),
        ),
        in_specs=[vmem] * 10 + [pl.BlockSpec(memory_space=pltpu.SMEM)] + [vmem] * 2,
        out_specs=(vmem, vmem),
        scratch_shapes=[
            pltpu.VMEM((model, 2 * HEAD), BF),
            pltpu.VMEM((model, 5 * HEAD), BF),
            pltpu.VMEM((model, 3 * HEAD), BF),
            pltpu.VMEM((rows, model), BF),
            pltpu.VMEM((n_tp, 8, rows), F32),
            pltpu.VMEM((2, rows + 2 * RADIUS, HEAD), BF),
            pltpu.VMEM((n, 3, part, HEAD), BF),
            pltpu.VMEM((n, 3, part, HEAD), BF),
            pltpu.VMEM((3, part, HEAD), BF),
            pltpu.VMEM((n, 3, part, HEAD), BF),
            pltpu.VMEM((n, 2, part, HEAD), BF),
            pltpu.VMEM((n, 2, part, HEAD), BF),
            pltpu.VMEM((n, 2, part, HEAD), F32),
            pltpu.VMEM((5, rows, HEAD), BF),
            pltpu.VMEM((rows, rows), F32),
            pltpu.VMEM((2, rows, HEAD), F32),
            pltpu.VMEM((rows, HEAD), F32),
            pltpu.VMEM((2, rows, HEAD), F32),
            pltpu.VMEM((rows, 3 * HEAD), BF),
            pltpu.VMEM((n, CORES, nx, mine, size), BF),
            pltpu.VMEM((n, nx, mine, size), BF),
            pltpu.VMEM((n, nx, mine, size), BF),
            pltpu.VMEM((n, 3, mine, size), BF),
            dma((3,)),
            dma((3, n * n)),
            dma((8,)),
            dma((8,)),
            dma((n_tp - 1,)),
            dma((n_tp - 1,)),
            dma((2,)),
            dma((2,)),
            dma((n - 1,)),
            dma((n - 1,)),
            dma((n - 1,)),
            dma((n - 1,)),
            dma((n - 1,)),
            dma((n - 1,)),
            dma((n,)),
            dma((n,)),
            dma((n, 6)),
            dma((n, 6)),
        ],
        compiler_params=pltpu.CompilerParams(
            collective_id=0, has_side_effects=True, vmem_limit_bytes=56 * 1024 * 1024
        ),
    )(
                tokens,
        gain.reshape(1, width),
        qa,
        ka,
        va,
        qr,
        kr,
        vr,
        oa.T,
        orr.T,
        sink,
        decay,
        freqs,
    )


SP = ("sp_0", "sp_1")


def solution(mesh):
    n_tp = mesh.shape["tp"]
    n = round(mesh.shape["sp"] ** 0.5)
    finer = Mesh(mesh.devices.reshape(n, n, n_tp), ("sp_0", "sp_1", "tp"))
    return jax.shard_map(
        functools.partial(layer, n, n_tp),
        mesh=finer,
        in_specs=(
            P(SP, "tp"),
            P("tp"),
            P(SP, "tp"),
            P(SP, "tp"),
            P(SP, "tp"),
            P(SP, "tp"),
            P(SP, "tp"),
            P(SP, "tp"),
            P("tp", SP),
            P("tp", SP),
            P("tp"),
            P("tp", SP),
        ),
        out_specs=(P(("sp_0", "sp_1", "tp"), None), P("tp", SP)),
        check_vma=False,
    )
```

```python
import functools

import jax
import jax.numpy as jnp
from jax import lax
from jax.experimental import pallas as pl
from jax.experimental.pallas import tpu as pltpu
from jax.sharding import Mesh
from jax.sharding import PartitionSpec as P

HEAD = 128
RADIUS = 128
CORES = 2
MESH = pl.DeviceIdType.MESH
BF = jnp.bfloat16
F32 = jnp.float32

NT = (((1,), (1,)), ((), ()))

(
    PEERS, FIRST, SET_OUT, HOP, TOKENS_OUT, TOKENS_ON, TOKENS_FAR, TOKENS_IN, DECAYS,
    ANGLES, STATES, ALONG_Y, ALONG_Z, PROJECT_KEYS, PROJECT_QUERIES, PROJECT_RETENTION,
    RETENTION, ATTENTION, PARTIAL_SUMS, CORE_SUMS, X_SUMS, LAST_SUMS, DRAIN,
) = range(23)
ORDER = (
    (PEERS,), (FIRST, 0, 0), (SET_OUT, 0, 0), (FIRST, 1, 0), (SET_OUT, 1, 0), (FIRST, 2, 0),
    (TOKENS_OUT,), (DECAYS,), (ANGLES,), (FIRST, 0, 1), (SET_OUT, 0, 1), (HOP, 0, 1, 0),
    (FIRST, 1, 1), (SET_OUT, 1, 1), (FIRST, 2, 1), (HOP, 1, 1, 0), (FIRST, 0, 2),
    (SET_OUT, 0, 2), (TOKENS_ON,), (HOP, 0, 1, 1), (HOP, 0, 2, 0), (FIRST, 1, 2),
    (SET_OUT, 1, 2), (HOP, 1, 1, 1), (FIRST, 2, 2), (FIRST, 0, 3), (SET_OUT, 0, 3),
    (HOP, 0, 1, 2), (HOP, 0, 2, 1), (HOP, 0, 3, 0), (FIRST, 1, 3), (SET_OUT, 1, 3),
    (HOP, 1, 1, 2), (FIRST, 0, 4), (SET_OUT, 0, 4), (FIRST, 2, 3), (HOP, 1, 2, 0),
    (HOP, 0, 1, 3), (HOP, 0, 2, 2), (HOP, 0, 3, 1), (HOP, 0, 4, 0), (FIRST, 1, 4),
    (SET_OUT, 1, 4), (TOKENS_FAR,), (HOP, 1, 1, 3), (HOP, 1, 2, 1), (FIRST, 2, 4),
    (HOP, 1, 2, 2), (HOP, 0, 1, 4), (HOP, 0, 2, 3), (HOP, 0, 3, 2), (HOP, 0, 4, 1),
    (HOP, 1, 1, 4), (HOP, 1, 2, 3), (HOP, 1, 3, 0), (HOP, 0, 2, 4), (HOP, 0, 3, 3),
    (HOP, 0, 4, 2), (HOP, 1, 2, 4), (HOP, 1, 3, 1), (SET_OUT, 2, 0), (SET_OUT, 2, 1),
    (HOP, 0, 3, 4), (HOP, 0, 4, 3), (SET_OUT, 2, 2), (HOP, 1, 3, 2), (SET_OUT, 2, 3),
    (SET_OUT, 2, 4), (HOP, 1, 3, 3), (HOP, 1, 3, 4), (HOP, 0, 4, 4), (TOKENS_IN,), (STATES,),
    (HOP, 1, 4, 0), (HOP, 1, 4, 1), (HOP, 2, 1, 0), (HOP, 2, 1, 1), (HOP, 1, 4, 2),
    (HOP, 2, 1, 2), (HOP, 1, 4, 3), (HOP, 2, 1, 3), (HOP, 2, 1, 4), (ALONG_Y,), (HOP, 1, 4, 4),
    (PROJECT_KEYS,), (HOP, 2, 2, 0), (HOP, 2, 2, 1), (PROJECT_QUERIES,), (HOP, 2, 2, 2),
    (HOP, 2, 2, 3), (HOP, 2, 2, 4), (PROJECT_RETENTION,), (HOP, 2, 3, 0), (HOP, 2, 3, 1),
    (ATTENTION, 0), (ALONG_Z,), (HOP, 2, 3, 2), (ATTENTION, 1), (HOP, 2, 3, 3), (HOP, 2, 3, 4),
    (HOP, 2, 4, 0), (HOP, 2, 4, 1), (RETENTION,), (HOP, 2, 4, 2), (HOP, 2, 4, 3),
    (HOP, 2, 4, 4), (PARTIAL_SUMS, 0), (PARTIAL_SUMS, 1), (CORE_SUMS, 0), (PARTIAL_SUMS, 2),
    (CORE_SUMS, 1), (PARTIAL_SUMS, 3), (CORE_SUMS, 2), (PARTIAL_SUMS, 4), (CORE_SUMS, 3),
    (PARTIAL_SUMS, 5), (CORE_SUMS, 4), (PARTIAL_SUMS, 6), (CORE_SUMS, 5), (PARTIAL_SUMS, 7),
    (X_SUMS, 0), (CORE_SUMS, 6), (X_SUMS, 1), (CORE_SUMS, 7), (X_SUMS, 2), (X_SUMS, 3),
    (X_SUMS, 4), (X_SUMS, 5), (X_SUMS, 6), (X_SUMS, 7), (LAST_SUMS, 0), (LAST_SUMS, 1),
    (LAST_SUMS, 2), (LAST_SUMS, 3), (LAST_SUMS, 4), (LAST_SUMS, 5), (LAST_SUMS, 6),
    (LAST_SUMS, 7), (DRAIN,),
)


def dot(a, b, dims=None):
    if dims is None:
        return jnp.dot(a, b, preferred_element_type=F32)
    return lax.dot_general(a, b, dims, preferred_element_type=F32)


def column(row, lanes):
    return jnp.broadcast_to(row, (lanes, row.shape[1])).T


def row_of(col):
    return jnp.broadcast_to(col, (col.shape[0], HEAD)).T[0:1]


def layer_kernel(
    n,
    n_tp,
    tok_ref,
    gain_ref,
    qa_ref,
    ka_ref,
    va_ref,
    qr_ref,
    kr_ref,
    vr_ref,
    oa_ref,
    or_ref,
    sink_ref,
    decay_ref,
    freq_ref,
    mixed_ref,
    logw_ref,
    w1,
    w2,
    w3,
    tok,
    ssq,
    kv,
    st1,
    r1,
    st2,
    r2,
    st3,
    r3,
    pre,
    ret,
    dmat,
    tlead,
    inv,
    turns,
    heads,
    pbuf,
    dbuf,
    sbuf,
    rbuf,
    ssem,
    rsem,
    tsend,
    trecv,
    qsend,
    qrecv,
    hsend,
    hrecv,
    e1send,
    e1recv,
    e2send,
    e2recv,
    e3send,
    e3recv,
    dsend,
    drecv,
    xsend,
    xrecv,
    tok_own,
    gain_own,
    decay_own,
    freq_own,
    loaded,
):
    nx = n_tp // CORES
    rows, width = tok_ref.shape
    model = width * n_tp
    block = qa_ref.shape[0]
    z, y, t = lax.axis_index("sp_0"), lax.axis_index("sp_1"), lax.axis_index("tp")
    x, core = lax.div(t, CORES), lax.rem(t, CORES)
    sp = z * n + y
    half = n // 2
    flip = core == 0

    def wrap(i, m):
        return lax.rem(i + 2 * m, m)

    def place():
        return jnp.where(flip, y, z), jnp.where(flip, z, y)

    def at(a_to, b_to):
        return {"sp_0": jnp.where(flip, b_to, a_to), "sp_1": jnp.where(flip, a_to, b_to)}

    def tp_of(x_to, core_to):
        return {"tp": x_to * CORES + core_to}

    def remote(src, dst, send, recv, device):
        return pltpu.make_async_remote_copy(
            src_ref=src,
            dst_ref=dst,
            send_sem=send,
            recv_sem=recv,
            device_id=device,
            device_id_type=MESH,
        )

    partner = tp_of(x, 1 - core)
    after = wrap(sp + 1, n * n)
    before = wrap(sp - 1, n * n)
    next_dev = {"sp_0": lax.div(after, n), "sp_1": lax.rem(after, n)}
    prev_dev = {"sp_0": lax.div(before, n), "sp_1": lax.rem(before, n)}

    barrier = pltpu.get_barrier_semaphore()
    for k in range(1, n):
        pl.semaphore_signal(barrier, 1, device_id={"sp_1": wrap(y + k, n)}, device_id_type=MESH)
        pl.semaphore_signal(barrier, 1, device_id={"sp_0": wrap(z + k, n)}, device_id_type=MESH)
    for k in range(1, n_tp):
        pl.semaphore_signal(barrier, 1, device_id={"tp": wrap(t + k, n_tp)}, device_id_type=MESH)
    pl.semaphore_signal(barrier, 1, device_id=next_dev, device_id_type=MESH)
    pl.semaphore_signal(barrier, 1, device_id=prev_dev, device_id_type=MESH)

    cols = oa_ref.shape[0]
    own = pl.ds(pl.multiple_of(sp * block, block), block)
    own_out = pl.ds(pl.multiple_of(sp * cols, cols), cols)

    def heads_at(k, count=1):
        return pl.ds(k * HEAD, count * HEAD)

    moves = (
        (kr_ref, w1.at[own, heads_at(0)]),
        (vr_ref, w1.at[own, heads_at(1)]),
        (ka_ref, w2.at[own, heads_at(0)]),
        (va_ref, w2.at[own, heads_at(1)]),
        (qa_ref, w2.at[own, heads_at(2, 2)]),
        (qr_ref, w2.at[own, heads_at(4)]),
        (oa_ref, w3.at[own_out, heads_at(0, 2)]),
        (or_ref, w3.at[own_out, heads_at(2)]),
        (tok_ref, tok_own),
        (gain_ref, gain_own),
        (decay_ref, decay_own),
        (freq_ref, freq_own),
    )
    loads = [
        pltpu.make_async_copy(src, dst, loaded.at[k]) for k, (src, dst) in enumerate(moves)
    ]
    for load in loads:
        load.start()

    groups = ((w1, block), (w2, block), (w3, cols))

    def ring_send(g, a_from, b_from, device, h, k):
        buffer, size = groups[g]
        index = jnp.where(flip, b_from * n + a_from, a_from * n + b_from)
        ref = buffer.at[pl.ds(pl.multiple_of(index * size, size), size)]
        remote(ref, ref, ssem.at[g], rsem.at[g, h, k], device).start()

    def ring_take(g, count, h, k):
        buffer, size = groups[g]
        arrived(buffer.at[pl.ds(0, count * size)], rsem.at[g, h, k])

    def steps(k):
        a, _ = place()
        if k == 0:
            return [(0, a)]
        if k > half:
            return []
        up = [(2 * k - 1, wrap(a - k, n))]
        return up + [(2 * k, wrap(a + k, n))] if k < half else up

    def first(g, k):
        if k > half:
            return
        a, b = place()
        if k > 0:
            ring_take(g, len(steps(k)), 0, k)
        if k < half:
            ring_send(g, wrap(a - k, n), b, at(wrap(a + 1, n), b), 0, k + 1)
        if k < half - 1:
            ring_send(g, wrap(a + k, n), b, at(wrap(a - 1, n), b), 0, k + 1)

    def set_out(g, k):
        hop(g, 0, k)

    def hop(g, h, k):
        if h > half:
            return
        a, b = place()
        flows = []
        for i, a_from in steps(k):
            hops_up = half if i < half else half - 1
            flows += [(hops_up, 1, a_from), (n - 1 - hops_up, -1, a_from)]
        if h > 0 and flows:
            ring_take(g, sum(hops >= h for hops, _, _ in flows), h, k)
        for hops, way, a_from in flows:
            if hops > h:
                ring_send(g, a_from, wrap(b - way * h, n), at(a, wrap(b + way, n)), h + 1, k)

    def ring_done(g):
        buffer, size = groups[g]
        everything = buffer.at[pl.ds(0, (n * n - 1) * size)]
        remote(everything, everything, ssem.at[g], ssem.at[g], partner).wait_send()

    def wait_peers():
        pl.semaphore_wait(barrier, 2 * (n - 1) + (n_tp - 1) + 2)
        for load in loads[:8]:
            load.wait()


    def send(copy):
        copy.start()

    def arrived(ref, sem):
        remote(ref, ref, sem, sem, partner).wait_recv()

    def left(ref, sem):
        remote(ref, ref, sem, sem, partner).wait_send()

    def token_slot(t_from):
        return pl.ds(pl.multiple_of(t_from * width, width), width)

    def token_copy(k, t_from, device, part=None):
        ref = tok.at[:, token_slot(t_from)]
        if part is not None:
            ref = tok.at[pl.ds(part * (rows // 2), rows // 2), token_slot(t_from)]
        return remote(ref, ref, tsend.at[0], trecv.at[k], device)

    x_up, x_down, x_far = wrap(x + 1, nx), wrap(x - 1, nx), wrap(x + 2, nx)

    def tokens_out():
        loads[8].wait()
        loads[9].wait()
        widened = tok_own[...].astype(F32)
        tok[:, token_slot(t)] = (widened * gain_own[...]).astype(BF)
        ssq[t] = jnp.broadcast_to(
            row_of(jnp.sum(widened * widened, axis=1, keepdims=True)), (8, rows)
        )
        send(token_copy(0, t, partner))
        if nx == 4:
            send(token_copy(1, t, tp_of(x_up, core)))
            send(token_copy(2, t, tp_of(x_down, core)))
        for k in range(1, n_tp):
            there = {"tp": wrap(t + k, n_tp)}
            send(remote(ssq.at[t], ssq.at[t], qsend.at[0], qrecv.at[0], there))

    def tokens_on():
        if nx == 4:
            from_down, from_up = x_down * CORES + core, x_up * CORES + core
            token_copy(1, from_down, partner).wait_recv()
            send(token_copy(3, from_down, tp_of(x_up, core), 0))
            send(token_copy(5, from_down, partner))
            token_copy(2, from_up, partner).wait_recv()
            send(token_copy(4, from_up, tp_of(x_down, core), 1))
            send(token_copy(6, from_up, partner))

    def tokens_far():
        if nx == 4:
            from_far = x_far * CORES + core
            token_copy(3, from_far, partner, 0).wait_recv()
            token_copy(4, from_far, partner, 1).wait_recv()
            send(token_copy(7, from_far, partner))

    def tokens_in():
        token_copy(0, x * CORES + 1 - core, partner).wait_recv()
        if nx == 4:
            for k, x_from in ((5, x_down), (6, x_up), (7, x_far)):
                token_copy(k, x_from * CORES + 1 - core, partner).wait_recv()
        arrived(ssq.at[pl.ds(0, n_tp - 1)], qrecv.at[0])
        squares = ssq[0]
        for k in range(1, n_tp):
            squares = squares + ssq[k]
        inv[...] = column(lax.rsqrt(squares[0:1] / model + 1e-06), HEAD)

    def decays():
        loads[10].wait()
        ii = lax.broadcasted_iota(jnp.int32, (rows, rows), 0)
        jj = lax.broadcasted_iota(jnp.int32, (rows, rows), 1)
        cumul = jnp.sum(jnp.where(jj <= ii, decay_own[...], 0.0), axis=1, keepdims=True)
        cumul_row = row_of(cumul)
        last = cumul_row[:, rows - 1 : rows]
        dmat[...] = jnp.exp(-jnp.abs(cumul - cumul_row))
        tlead[0] = jnp.broadcast_to(jnp.exp(last - cumul), (rows, HEAD))
        tlead[1] = jnp.broadcast_to(jnp.exp(cumul), (rows, HEAD))
        st1[:, 2] = jnp.broadcast_to(spread(last)[None], (n, part, HEAD))

    part = HEAD // n

    def spread(total):
        high = jnp.broadcast_to(total, (part, HEAD)).astype(BF).astype(F32)
        low = jnp.broadcast_to(total, (part, HEAD)) - high
        line = lax.broadcasted_iota(jnp.int32, (part, HEAD), 0)
        return jnp.where(line == 0, high, jnp.where(line == 1, low, 0.0)).astype(BF)

    def gathered(tile):
        return jnp.sum(tile[0:2].astype(F32), axis=0, keepdims=True)

    def states():
        first_part = dot(tok[...], w1[...])
        inverse = inv[...]
        ret_key = (first_part[:, 0:HEAD] * (inverse * HEAD ** (-0.5))).astype(BF)
        ret_value = (first_part[:, HEAD:] * inverse).astype(BF)
        ret[0] = ret_key
        ret[1] = ret_value
        key_f = ret_key.astype(F32)
        turned = jnp.concatenate([(key_f * tlead[0]).T, (key_f * tlead[1]).T], axis=0)
        both = dot(turned.astype(BF), ret_value)
        st1[:, 0] = both[0:HEAD].reshape(n, part, HEAD).astype(BF)
        st1[:, 1] = both[HEAD:].reshape(n, part, HEAD).astype(BF)
        for k in range(1, n):
            y_to = wrap(y + k, n)
            there = {"sp_1": y_to}
            send(remote(st1.at[y_to], r1.at[y], e1send.at[0], e1recv.at[0], there))
        r1[y] = st1[y]

    def along_y():
        arrived(r1.at[pl.ds(0, n - 1)], e1recv.at[0])
        logs = [gathered(r1[k, 2]) for k in range(n)]
        total = logs[0]
        for k in range(1, n):
            total = total + logs[k]
        fades = [jnp.exp(v) for v in logs]
        ahead = jnp.zeros((part, HEAD), F32)
        for k in range(n):
            pre[k, 0] = ahead
            ahead = fades[k] * ahead + r1[k, 0].astype(F32)
        behind = jnp.zeros((part, HEAD), F32)
        for k in reversed(range(n)):
            pre[k, 1] = behind
            behind = fades[k] * behind + r1[k, 1].astype(F32)
        st2[0] = ahead.astype(BF)
        st2[1] = behind.astype(BF)
        st2[2] = spread(total)
        for k in range(1, n):
            there = {"sp_0": wrap(z + k, n)}
            send(remote(st2, r2.at[z], e2send.at[0], e2recv.at[0], there))

    def along_z():
        arrived(r2.at[pl.ds(0, n - 1)], e2recv.at[0])
        r2[z] = st2[...]
        fades = [jnp.exp(gathered(r1[k, 2])) for k in range(n)]
        ahead = jnp.zeros((part, HEAD), F32)
        for k in range(n - 1):
            moved = jnp.exp(gathered(r2[k, 2])) * ahead + r2[k, 0].astype(F32)
            ahead = jnp.where(k < z, moved, ahead)
        behind = jnp.zeros((part, HEAD), F32)
        for k in reversed(range(1, n)):
            moved = jnp.exp(gathered(r2[k, 2])) * behind + r2[k, 1].astype(F32)
            behind = jnp.where(k > z, moved, behind)
        for k in range(n):
            st3[k, 0] = (pre[k, 0] + ahead).astype(BF)
            ahead = ahead * fades[k]
        for k in reversed(range(n)):
            st3[k, 1] = (pre[k, 1] + behind).astype(BF)
            behind = behind * fades[k]
        for k in range(1, n):
            y_to = wrap(y + k, n)
            there = {"sp_1": y_to}
            send(remote(st3.at[y_to], r3.at[y], e3send.at[0], e3recv.at[0], there))
        r3[y] = st3[y]

    to_next = remote(
        kv.at[:, pl.ds(rows, RADIUS)],
        kv.at[:, pl.ds(0, RADIUS)],
        hsend.at[0],
        hrecv.at[0],
        next_dev,
    )
    to_prev = remote(
        kv.at[:, pl.ds(RADIUS, RADIUS)],
        kv.at[:, pl.ds(RADIUS + rows, RADIUS)],
        hsend.at[0],
        hrecv.at[1],
        prev_dev,
    )

    def rotated(v):
        return v * turns[0] + pltpu.roll(v, HEAD // 2, 1) * turns[1]

    def angles():
        loads[11].wait()
        position = lax.broadcasted_iota(jnp.int32, (rows, HEAD), 0) + sp * rows
        angle = position.astype(F32) * freq_own[...]
        second_half = lax.broadcasted_iota(jnp.int32, (rows, HEAD), 1) >= HEAD // 2
        sine = jnp.sin(angle)
        turns[0] = jnp.cos(angle)
        turns[1] = jnp.where(second_half, sine, -sine)

    def project_keys():
        both = dot(tok[...], w2[:, 0 : 2 * HEAD])
        kv[0, RADIUS : RADIUS + rows] = rotated(both[:, :HEAD] * inv[...]).astype(BF)
        kv[1, RADIUS : RADIUS + rows] = (both[:, HEAD:] * inv[...]).astype(BF)
        send(to_next)
        send(to_prev)

    def project_queries():
        both = dot(tok[...], w2[:, 2 * HEAD : 4 * HEAD])
        for k in range(2):
            own_head = both[:, k * HEAD : (k + 1) * HEAD]
            ret[3 + k] = rotated(own_head * inv[...]).astype(BF)

    def project_retention():
        ret[2] = (dot(tok[...], w2[:, 4 * HEAD :]) * inv[...]).astype(BF)

    def retention():
        arrived(r3.at[pl.ds(0, n - 1)], e3recv.at[0])
        ret_query = ret[2]
        weights = (dot(ret_query, ret[0], NT) * dmat[...]).astype(BF)
        mix = dot(weights, ret[1])
        mix = mix + tlead[1] * dot(ret_query, r3[:, 0].reshape(HEAD, HEAD))
        mix = mix + tlead[0] * dot(ret_query, r3[:, 1].reshape(HEAD, HEAD))
        middle = mix - jnp.mean(mix, axis=1, keepdims=True)
        normed = middle * lax.rsqrt(jnp.mean(middle * middle, axis=1, keepdims=True) + 1e-06)
        heads[:, 2 * HEAD :] = normed.astype(BF)

    def attention(k):
        if k == 0:
            to_next.wait_recv()
            to_prev.wait_recv()
        span = rows + 2 * RADIUS
        query_at = lax.broadcasted_iota(jnp.int32, (rows, span), 0)
        key_at = lax.broadcasted_iota(jnp.int32, (rows, span), 1) - RADIUS
        key_pos = key_at + sp * rows
        valid = (
            (jnp.abs(key_at - query_at) <= RADIUS) & (key_pos >= 0) & (key_pos < n * n * rows)
        )
        scores = dot(ret[3 + k], kv[0], NT) * HEAD ** (-0.5)
        masked = jnp.where(valid, scores, -jnp.inf)
        sink = sink_ref[k]
        top = jnp.maximum(jnp.max(masked, axis=1, keepdims=True), sink)
        expo = jnp.exp(masked - top)
        total = jnp.sum(expo, axis=1, keepdims=True) + jnp.exp(sink - top)
        logw_ref[k : k + 1, :] = row_of(top + jnp.log(total))
        probs = (expo * (1.0 / total)).astype(BF)
        heads[:, k * HEAD : (k + 1) * HEAD] = dot(probs, kv[1]).astype(BF)

    size = model // n
    mine = rows // n_tp
    half_1, half_2 = pl.ds(0, size // 2), pl.ds(size // 2, size // 2)

    def core_copy(c):
        return remote(pbuf.at[c, 1 - core], dbuf.at[c], dsend.at[0], drecv.at[c], partner)

    def x_copy(c, k):
        up = k in (0, 2, 4)
        x_to = (x_far, x_far, x_up, x_down, x_up, x_down)[k]
        columns = (half_1, half_2, half_1, half_2, half_2, half_1)[k]
        return remote(
            sbuf.at[c, x_to, :, columns],
            rbuf.at[c, k // 2, :, half_1 if up else half_2]
            if k < 2
            else rbuf.at[c, 1 if up else 2, :, columns],
            xsend.at[0],
            xrecv.at[c, 0 if k < 2 else 1],
            tp_of(x_up if up else x_down, core),
        )

    def columns_of(c):
        return pl.ds(c * size, size)

    def partial_sums(c):
        if c >= n:
            return
        partial = dot(heads[...], w3[columns_of(c)], NT)
        parted = partial.astype(BF).reshape(nx, CORES, mine, size)
        for k in range(CORES):
            pbuf[c, k] = parted[:, k]
        send(core_copy(c))

    def core_sums(c):
        if c >= n:
            return
        core_copy(c).wait_recv()
        sbuf[c] = (pbuf[c, core].astype(F32) + dbuf[c].astype(F32)).astype(BF)
        if nx == 4:
            for k in (0, 1, 4, 5) if c < n // 2 else (0, 1):
                send(x_copy(c, k))

    def x_sums(c):
        if nx == 4 and c < n:
            arrived(rbuf.at[c, 0], xrecv.at[c, 0])
            passed = rbuf[c, 0, :, 0 : size // 2].astype(F32)
            sbuf[c, x_up, :, 0 : size // 2] = (
                sbuf[c, x_up, :, 0 : size // 2].astype(F32) + passed
            ).astype(BF)
            send(x_copy(c, 2))
            passed = rbuf[c, 0, :, size // 2 :].astype(F32)
            sbuf[c, x_down, :, size // 2 :] = (
                sbuf[c, x_down, :, size // 2 :].astype(F32) + passed
            ).astype(BF)
            send(x_copy(c, 3))
            if c >= n // 2:
                send(x_copy(c, 4))
                send(x_copy(c, 5))

    def last_sums(c):
        if c >= n:
            return
        result = sbuf[c, x].astype(F32)
        if nx == 4:
            arrived(rbuf.at[c, pl.ds(1, 2)], xrecv.at[c, 1])
            result = result + rbuf[c, 1].astype(F32) + rbuf[c, 2].astype(F32)
        mixed_ref[:, columns_of(c)] = result.astype(BF)

    def drain():
        for g in range(3):
            ring_done(g)
        left(ssq.at[pl.ds(0, n_tp - 1)], qsend.at[0])
        left(tok.at[:, pl.ds(0, (n_tp - 1) * width)], tsend.at[0])
        left(kv.at[:, pl.ds(0, 2 * RADIUS)], hsend.at[0])
        left(r1.at[pl.ds(0, n - 1)], e1send.at[0])
        left(r2.at[pl.ds(0, n - 1)], e2send.at[0])
        left(r3.at[pl.ds(0, n - 1)], e3send.at[0])
        left(dbuf, dsend.at[0])
        if nx == 4:
            left(rbuf, xsend.at[0])

    stages = (
        wait_peers,
        first,
        set_out,
        hop,
        tokens_out,
        tokens_on,
        tokens_far,
        tokens_in,
        decays,
        angles,
        states,
        along_y,
        along_z,
        project_keys,
        project_queries,
        project_retention,
        retention,
        attention,
        partial_sums,
        core_sums,
        x_sums,
        last_sums,
        drain,
    )
    for code, *numbers in ORDER:
        stages[code](*numbers)


def layer(n, n_tp, *args):
    tokens, gain, qa, ka, va, qr, kr, vr, oa, orr, sink, decay = args
    rows, width = tokens.shape
    model = width * n_tp
    freqs = 10000.0 ** (-jnp.arange(0, HEAD, 2).astype(F32) / HEAD)
    freqs = jnp.concatenate([freqs, freqs]).reshape(1, HEAD)
    nx = n_tp // CORES
    part = HEAD // n
    size = model // n
    mine = rows // n_tp
    vmem = pl.BlockSpec(memory_space=pltpu.VMEM)
    hbm = pl.BlockSpec(memory_space=pltpu.HBM)
    dma = pltpu.SemaphoreType.DMA
    return pl.pallas_call(
        functools.partial(layer_kernel, n, n_tp),
        name="layer",
        out_shape=(
            jax.ShapeDtypeStruct((mine, model), BF),
            jax.ShapeDtypeStruct((2, rows), F32),
        ),
        in_specs=[hbm] * 10 + [pl.BlockSpec(memory_space=pltpu.SMEM)] + [hbm] * 2,
        out_specs=(vmem, vmem),
        scratch_shapes=[
            pltpu.VMEM((model, 2 * HEAD), BF),
            pltpu.VMEM((model, 5 * HEAD), BF),
            pltpu.VMEM((model, 3 * HEAD), BF),
            pltpu.VMEM((rows, model), BF),
            pltpu.VMEM((n_tp, 8, rows), F32),
            pltpu.VMEM((2, rows + 2 * RADIUS, HEAD), BF),
            pltpu.VMEM((n, 3, part, HEAD), BF),
            pltpu.VMEM((n, 3, part, HEAD), BF),
            pltpu.VMEM((3, part, HEAD), BF),
            pltpu.VMEM((n, 3, part, HEAD), BF),
            pltpu.VMEM((n, 2, part, HEAD), BF),
            pltpu.VMEM((n, 2, part, HEAD), BF),
            pltpu.VMEM((n, 2, part, HEAD), F32),
            pltpu.VMEM((5, rows, HEAD), BF),
            pltpu.VMEM((rows, rows), F32),
            pltpu.VMEM((2, rows, HEAD), F32),
            pltpu.VMEM((rows, HEAD), F32),
            pltpu.VMEM((2, rows, HEAD), F32),
            pltpu.VMEM((rows, 3 * HEAD), BF),
            pltpu.VMEM((n, CORES, nx, mine, size), BF),
            pltpu.VMEM((n, nx, mine, size), BF),
            pltpu.VMEM((n, nx, mine, size), BF),
            pltpu.VMEM((n, 3, mine, size), BF),
            dma((3,)),
            dma((3, n // 2 + 1, n // 2 + 1)),
            dma((1,)),
            dma((8,)),
            dma((1,)),
            dma((1,)),
            dma((1,)),
            dma((2,)),
            dma((1,)),
            dma((1,)),
            dma((1,)),
            dma((1,)),
            dma((1,)),
            dma((1,)),
            dma((1,)),
            dma((n,)),
            dma((1,)),
            dma((n, 2)),
            pltpu.VMEM((rows, width), BF),
            pltpu.VMEM((1, width), F32),
            pltpu.VMEM((1, rows), F32),
            pltpu.VMEM((1, HEAD), F32),
            dma((12,)),
        ],
        compiler_params=pltpu.CompilerParams(
            collective_id=0, has_side_effects=True, vmem_limit_bytes=56 * 1024 * 1024
        ),
    )(
                tokens,
        gain.reshape(1, width),
        qa,
        ka,
        va,
        qr,
        kr,
        vr,
        oa.T,
        orr.T,
        sink,
        decay,
        freqs,
    )


SP = ("sp_0", "sp_1")


def solution(mesh):
    n_tp = mesh.shape["tp"]
    n = round(mesh.shape["sp"] ** 0.5)
    finer = Mesh(mesh.devices.reshape(n, n, n_tp), ("sp_0", "sp_1", "tp"))
    return jax.shard_map(
        functools.partial(layer, n, n_tp),
        mesh=finer,
        in_specs=(
            P(SP, "tp"),
            P("tp"),
            P(SP, "tp"),
            P(SP, "tp"),
            P(SP, "tp"),
            P(SP, "tp"),
            P(SP, "tp"),
            P(SP, "tp"),
            P("tp", SP),
            P("tp", SP),
            P("tp"),
            P("tp", SP),
        ),
        out_specs=(P(("sp_0", "sp_1", "tp"), None), P("tp", SP)),
        check_vma=False,
    )
```
